32 devices in a mesh: sp: 16 (over z, y, core), tp: 2 (over x).
Axes of the slice: x: 2, y: 2, z: 4, core: 2. Of those that a mesh axis runs over, the one named last changes fastest.
Arguments:
- incoming_activity: bfloat16 [8192, 2048], P(('sp', 'tp')), may hold values from -6 to 6
- entry_standardize_factor: bfloat16 [2048], replicated, may hold values from 0.099609375 to 1.8984375
- recursive_entry_matrix: bfloat16 [2048, 2048], P(None, 'tp'), may hold values from -0.125 to 0.125
- final_switch_matrix: bfloat16 [2048, 2048], P(None, 'tp'), may hold values from -0.125 to 0.125
- averaging_entry_matrix: bfloat16 [2048, 1024], P(None, 'tp'), may hold values from -0.125 to 0.125
- percolumn_filter_coefficients: bfloat16 [4, 2048], P(None, 'tp'), may hold values from -3 to 3
- switch_tiled_matrices: bfloat16 [2, 2, 32, 64, 64], P(None, None, 'tp'), may hold values from -0.75 to 0.75
- prior_fading_odds: float32 [2, 2048], P(None, 'tp'), may hold values from 2.7 to 17
- speed_factors: float32 [2, 8192], P(None, 'sp'), may hold values from 0.4 to 2.5, as said below
- extra_fading_amounts: float32 [2, 8192], P(None, 'sp'), may hold values from -1.39 to 0, as said below
- averaging_cluster_matrices: bfloat16 [8, 128, 128], P('tp'), may hold values from -0.5 to 0.5
- averaging_feature_factor: bfloat16 [1024], P('tp'), may hold values from 0.099609375 to 1.8984375
- recursive_final_matrix: bfloat16 [2048, 2048], P('tp'), may hold values from -0.25 to 0.25
- averaging_final_matrix: bfloat16 [1024, 2048], P('tp'), may hold values from -0.1875 to 0.1875
Outputs:
- mixed: bfloat16 [8192, 2048], P(('sp', 'tp'))
The draws below stay inside these ranges and needn't reach their ends.
Inputs may be any that keep to these rules, and one draw needn't show every extreme that they name: `speed_factors`: constant over each aligned block of 512 positions. `extra_fading_amounts`: each row has at most two nonzero entries.
All inputs are finite; a program needn't handle non-finite values.
Results may differ from the reference program's by a relative error of at most 0.017.
Values may be sent and summed in bfloat16 or wider, within the bound.
A program may use at most 128 MiB of HBM per device.

```python
import jax
import jax.numpy as jnp
from jax import lax

D = 2048
RG_BW = 64
POOL_GROUPS = 8
CONV_W = 4
TOK_SP = 512
D_RNN = 2048
D_POOL = 1024
RG_BLOCKS = 32
POOL_GW = 128
TOKENS = 8192


def draw_prior_fading_odds(key, part):
    pick_key, slow_key, fast_key = jax.random.split(jax.random.fold_in(key, 11), 3)
    share = 0.5
    slow = jax.random.uniform(pick_key, (2, D_RNN), jnp.float32) < share
    slow_rate = jnp.exp(jax.random.uniform(slow_key, (2, D_RNN), jnp.float32, jnp.log(0.004), jnp.log(0.04))) / TOKENS
    fast_rate = jnp.exp(jax.random.uniform(fast_key, (2, D_RNN), jnp.float32, jnp.log(0.02), jnp.log(0.06)))
    fading_speed = jnp.where(slow, slow_rate, fast_rate)
    return -jnp.log(jnp.expm1(fading_speed))


def draw_speed_factors(key, part):
    block_key = jax.random.fold_in(key, 23)
    blocks = TOKENS // TOK_SP
    factor = jnp.exp(jax.random.uniform(block_key, (2, blocks), jnp.float32, jnp.log(0.4), jnp.log(2.5)))
    return jnp.repeat(factor, TOK_SP, axis=1)


def draw_extra_fading_amounts(key, part):
    spot_key, size_key = jax.random.split(jax.random.fold_in(key, 37))
    spots = jax.random.randint(spot_key, (2, 2, 1), 0, TOKENS)
    sizes = jnp.log(jax.random.uniform(size_key, (2, 2, 1), jnp.float32, 0.5, 0.8))
    positions = jnp.arange(TOKENS)[None, None, :]
    return jnp.sum(jnp.where(positions == spots, sizes, 0.0), axis=1)


def level_of(own_key, extent, shards, least, largest):
    loudness = 1.0
    for axis_at, parts in shards:
        heights = jax.random.uniform(jax.random.fold_in(jax.random.fold_in(own_key, 6), axis_at), (parts,), jnp.float32, least / len(shards), largest / len(shards))
        loudness = loudness * jnp.repeat(jnp.exp(heights), extent[axis_at] // parts).reshape((-1,) + (1,) * (len(extent) - 1 - axis_at))
    return loudness


def centred(key, extent, width, most, cuts=(), dtype=jnp.bfloat16):
    array = width * jax.random.normal(key, extent, jnp.float32)
    if cuts:
        array = array * level_of(key, extent, cuts, -0.22, 0.18)
    return jnp.clip(array, -most, most).astype(dtype)


def setup_inputs(seed: int = 0) -> dict:
    arg_keys = jax.random.split(jax.random.key(seed), 15)
    return {
        "incoming_activity": centred(arg_keys[0], (TOKENS, D), 1.0, 6.0, ((0, 32),)),
        "entry_standardize_factor": jnp.clip(1.0 + 0.18 * jax.random.normal(arg_keys[1], (D,), jnp.float32), 0.099609375, 1.8984375).astype(jnp.bfloat16),
        "recursive_entry_matrix": centred(arg_keys[2], (D, D_RNN), D ** -0.5, 0.125, ((1, 2),)),
        "final_switch_matrix": centred(arg_keys[3], (D, D_RNN), D ** -0.5, 0.125, ((1, 2),)),
        "averaging_entry_matrix": centred(arg_keys[4], (D, D_POOL), D ** -0.5, 0.125, ((1, 2),)),
        "percolumn_filter_coefficients": centred(arg_keys[5], (CONV_W, D_RNN), CONV_W ** -0.5, 3.0, ((1, 2),)),
        "switch_tiled_matrices": centred(arg_keys[6], (2, 2, RG_BLOCKS, RG_BW, RG_BW), RG_BW ** -0.5, 0.75, ((2, 2),)),
        "prior_fading_odds": draw_prior_fading_odds(jax.random.fold_in(arg_keys[14], 71), 0),
        "speed_factors": draw_speed_factors(jax.random.fold_in(arg_keys[14], 71), 0),
        "extra_fading_amounts": draw_extra_fading_amounts(jax.random.fold_in(arg_keys[14], 71), 0),
        "averaging_cluster_matrices": centred(arg_keys[10], (POOL_GROUPS, POOL_GW, POOL_GW), POOL_GW ** -0.5, 0.5, ((0, 2),)),
        "averaging_feature_factor": jnp.clip(1.0 + 0.18 * jax.random.normal(arg_keys[11], (D_POOL,), jnp.float32), 0.099609375, 1.8984375).astype(jnp.bfloat16),
        "recursive_final_matrix": centred(arg_keys[12], (D_RNN, D), (D_RNN // 4) ** -0.5, 0.25, ((0, 2),)),
        "averaging_final_matrix": centred(arg_keys[13], (D_POOL, D), D_POOL ** -0.5, 0.1875, ((0, 2),)),
    }


FADING_FACTOR = 8.0
epsilon = 1e-06

def combine(earlier, later):
    return (earlier[0] * later[0], later[0] * earlier[1] + later[1])

def product(left, right):
    return jnp.dot(left, right, preferred_element_type=jnp.float32)

def reference(incoming_activity, entry_standardize_factor, recursive_entry_matrix, final_switch_matrix, averaging_entry_matrix, percolumn_filter_coefficients, switch_tiled_matrices, prior_fading_odds, speed_factors, extra_fading_amounts, averaging_cluster_matrices, averaging_feature_factor, recursive_final_matrix, averaging_final_matrix):
    values = incoming_activity.astype(jnp.float32)
    scaled = values * lax.rsqrt(lax.optimization_barrier(jnp.mean(values * values, axis=1, keepdims=True)) + epsilon)
    normed = (scaled * entry_standardize_factor.astype(jnp.float32)).astype(jnp.bfloat16)
    state_input = product(normed, recursive_entry_matrix).astype(jnp.bfloat16)
    gate_input = product(normed, final_switch_matrix).astype(jnp.bfloat16)
    pool_input = product(normed, averaging_entry_matrix).astype(jnp.bfloat16)
    length = incoming_activity.shape[0]
    padded = jnp.pad(state_input.astype(jnp.float32), ((2, 1), (0, 0)))
    filtered = percolumn_filter_coefficients[0].astype(jnp.float32) * padded[0:length]
    for shift in range(1, CONV_W):
        filtered = filtered + percolumn_filter_coefficients[shift].astype(jnp.float32) * padded[shift:shift + length]
    filtered = filtered.astype(jnp.bfloat16)
    filtered_wide = filtered.astype(jnp.float32)
    blocks = filtered_wide.reshape(length, RG_BLOCKS, RG_BW)
    state_sum = jnp.zeros((length, D_RNN), jnp.float32)
    for sweep_orientation in range(2):
        gate_sums = jnp.einsum('tbi,qbij->tqbj', blocks, switch_tiled_matrices[sweep_orientation].astype(jnp.float32)).reshape(length, 2, D_RNN)
        remember_switch = jax.nn.sigmoid(gate_sums[:, 0])
        inlet = jax.nn.sigmoid(gate_sums[:, 1])
        fading_speed = jax.nn.softplus(-prior_fading_odds[sweep_orientation])
        logarithmic_persistence = -FADING_FACTOR * speed_factors[sweep_orientation][:, None] * remember_switch * fading_speed[None, :] + extra_fading_amounts[sweep_orientation][:, None]
        drive = jnp.sqrt(-jnp.expm1(2.0 * logarithmic_persistence)) * inlet * filtered_wide
        unused, states = lax.associative_scan(combine, (jnp.exp(logarithmic_persistence), drive), axis=0, reverse=sweep_orientation == 1)
        state_sum = state_sum + states
    state_mix = (jax.nn.gelu(gate_input.astype(jnp.float32)) * state_sum).astype(jnp.bfloat16)
    pool_wide = pool_input.astype(jnp.float32)
    pool_padded = jnp.pad(pool_wide, ((8, 8), (0, 0)))
    positions = jnp.arange(length).astype(jnp.int32)
    groups = []
    for group in range(POOL_GROUPS):
        half = 2 ** (group % 4)
        first = group * POOL_GW
        total = jnp.zeros((length, POOL_GW), jnp.float32)
        for offset in range(2 * half):
            begin = 8 - half + offset
            total = total + pool_padded[begin:begin + length, first:first + POOL_GW]
        upper = jnp.minimum(positions + half, length)
        lower = jnp.maximum(positions - half, 0)
        counted = (upper - lower).astype(jnp.float32)[:, None]
        groups.append(total / counted - pool_wide[:, first:first + POOL_GW])
    pooled = jnp.concatenate(groups, axis=1).astype(jnp.bfloat16)
    grouped = jnp.einsum('tgi,gij->tgj', pooled.astype(jnp.float32).reshape(length, POOL_GROUPS, POOL_GW), averaging_cluster_matrices.astype(jnp.float32)).reshape(length, D_POOL)
    pool_mix = (grouped * averaging_feature_factor.astype(jnp.float32)).astype(jnp.bfloat16)
    return (product(state_mix, recursive_final_matrix) + product(pool_mix, averaging_final_matrix)).astype(jnp.bfloat16)
```

```python
import functools

import jax
import jax.numpy as jnp
from jax import lax
from jax.experimental import pallas as pl
from jax.experimental.pallas import tpu as pltpu
from jax.sharding import PartitionSpec as P

FADING_FACTOR = 8.0
epsilon = 1e-06
EDGE = 16
MESH = pl.DeviceIdType.MESH
F32 = jnp.float32
BF16 = jnp.bfloat16


def product(left, right):
    return jnp.dot(left, right, preferred_element_type=F32)


def sigmoid(x):
    return 1.0 / (1.0 + jnp.exp(-x))


def small_softplus(odds):
    e = jnp.exp(-odds)
    z = e / (2.0 + e)
    y = z * z
    return 2.0 * z * (1.0 + y * (1.0 / 3.0 + y * (1.0 / 5.0 + y * (1.0 / 7.0))))


def one_less_exp(y, exp_y):
    near = 1.0 + y * (1.0 / 6.0) * (1.0 + y * (1.0 / 7.0))
    near = 1.0 + y * (1.0 / 5.0) * near
    near = 1.0 + y * (1.0 / 4.0) * near
    near = 1.0 + y * (1.0 / 3.0) * near
    near = 1.0 + y * (1.0 / 2.0) * near
    return jnp.where(y > -0.25, -y * near, 1.0 - exp_y)


def kernel(
    n_sp,
    n_tp,
    x_hbm,
    gain_ref,
    ws_hbm,
    wg_hbm,
    wp_hbm,
    conv_ref,
    switch_ref,
    odds_ref,
    cols_ref,
    cluster_ref,
    factor_ref,
    wso_hbm,
    wpo_hbm,
    out_ref,
    x_own,
    x_far,
    halo,
    normed,
    ws,
    wg,
    wp,
    wso,
    wpo,
    s_buf,
    g_buf,
    p_buf,
    filt,
    diag,
    sums,
    keep,
    loc,
    summary,
    totals,
    mix,
    pool_mix,
    part,
    landed,
    w_sem,
    ag_send,
    ag_recv,
    halo_send,
    halo_recv,
    c_send,
    c_recv,
    rs_send,
    rs_recv,
):
    sp = lax.axis_index("sp")
    tp = lax.axis_index("tp")
    rows, depth = x_own.shape
    length = rows * n_tp
    width = ws.shape[1]
    pool_width = wp.shape[1]

    gathers = []
    nxt = lax.rem(sp + 1, n_sp)
    prv = lax.rem(sp + n_sp - 1, n_sp)

    def halo_copy(side, tp_to, slot):
        src = x_hbm.at[pl.ds(rows - EDGE if side == 0 else 0, EDGE)]
        return pltpu.make_async_remote_copy(
            src_ref=src,
            dst_ref=halo.at[side],
            send_sem=halo_send.at[side, slot],
            recv_sem=halo_recv.at[side],
            device_id=(nxt if side == 0 else prv, tp_to),
            device_id_type=MESH,
        )

    for side, sender in ((0, n_tp - 1), (1, 0)):

        @pl.when(tp == sender)
        def _():
            for j in range(n_tp):
                halo_copy(side, j, j).start()

    for k in range(1, n_tp):
        copy = pltpu.make_async_remote_copy(
            src_ref=x_hbm,
            dst_ref=x_far.at[pl.ds((k - 1) * rows, rows)],
            send_sem=ag_send.at[k],
            recv_sem=ag_recv.at[k],
            device_id=(sp, lax.rem(tp + k, n_tp)),
            device_id_type=MESH,
        )
        copy.start()
        gathers.append(copy)
    loads = []
    for i, (src, dst) in enumerate(
        (
            (x_hbm, x_own),
            (ws_hbm, ws),
            (wg_hbm, wg),
            (wp_hbm, wp),
            (wso_hbm, wso),
            (wpo_hbm, wpo),
        )
    ):
        copy = pltpu.make_async_copy(src, dst, w_sem.at[i])
        copy.start()
        loads.append(copy)

    gain = gain_ref[...].astype(F32)

    def normalise(src, count, at):
        @pl.loop(0, count // 16)
        def _(i):
            at_row = pl.multiple_of(i * 16, 16)
            values = src[pl.ds(at_row, 16), :].astype(F32)
            mean = jnp.mean(values * values, axis=1, keepdims=True)
            scaled = values * lax.rsqrt(mean + epsilon)
            normed[pl.ds(pl.multiple_of(at + at_row, 16), 16), :] = (scaled * gain).astype(BF16)

    tile = min(256, width)
    ptile = min(256, pool_width)

    def owner_row(k):
        return pl.multiple_of(EDGE + lax.rem(tp + n_tp - k, n_tp) * rows, 16)

    def project(weights, buf, step, first, count, pieces, act):
        @pl.loop(0, weights.shape[1] // step)
        def _(c):
            at = pl.ds(pl.multiple_of(c * step, step), step)
            value = product(normed[pl.ds(first, count), :], weights[:, at]).astype(BF16)
            value = act(value.astype(F32))
            for begin, size, row in pieces:
                buf[pl.ds(row, size), at] = value[begin : begin + size]

    same = lambda v: v
    gelu = functools.partial(jax.nn.gelu, approximate=True)

    half = switch_ref.shape[2]
    spread = (
        lax.broadcasted_iota(jnp.int32, (half, tile), 1) % half
        == lax.broadcasted_iota(jnp.int32, (half, tile), 0)
    ).astype(F32).astype(BF16)
    on_diag = (
        lax.broadcasted_iota(jnp.int32, (tile, tile), 0) // half
        == lax.broadcasted_iota(jnp.int32, (tile, tile), 1) // half
    )
    for m in range(4):

        @pl.loop(0, width // tile)
        def _(g):
            at = pl.ds(pl.multiple_of(g * tile, tile), tile)
            wide = product(switch_ref[m, at, :], spread)
            diag[m, at, :] = jnp.where(on_diag, wide, 0.0).astype(BF16)

    loads[0].wait()
    normalise(x_own, rows, 0)
    own = ((0, rows, owner_row(0)),)
    loads[1].wait()
    project(ws, s_buf, tile, 0, rows, own, same)
    loads[2].wait()
    project(wg, g_buf, tile, 0, rows, own, gelu)
    loads[3].wait()
    project(wp, p_buf, ptile, 0, rows, own, same)

    far = rows * (n_tp - 1)
    for side in range(2):
        halo_copy(side, 0, 0).wait_recv()
    normalise(halo.at[0], EDGE, rows + far)
    normalise(halo.at[1], EDGE, rows + far + EDGE)

    @pl.when(sp == 0)
    def _():
        normed[pl.ds(rows + far, EDGE), :] = jnp.zeros((EDGE, depth), BF16)

    @pl.when(sp == n_sp - 1)
    def _():
        normed[pl.ds(rows + far + EDGE, EDGE), :] = jnp.zeros((EDGE, depth), BF16)

    for copy in gathers:
        copy.wait_recv()
    normalise(x_far, far, rows)
    pieces = [((k - 1) * rows, rows, owner_row(k)) for k in range(1, n_tp)]
    edges = [(far, EDGE, 0), (far + EDGE, EDGE, EDGE + length)]
    project(ws, s_buf, tile, rows, far + 2 * EDGE, pieces + edges, same)

    total_rows = length + 2 * EDGE

    @pl.loop(0, width // tile)
    def _(g):
        at = pl.ds(pl.multiple_of(g * tile, tile), tile)
        taps = conv_ref[:, at].astype(F32)
        x = s_buf[:, at]
        y = taps[0:1] * pltpu.roll(x, 2, 0)
        y = y + taps[1:2] * pltpu.roll(x, 1, 0)
        y = y + taps[2:3] * x
        y = y + taps[3:4] * pltpu.roll(x, total_rows - 1, 0)
        y = y[EDGE : EDGE + length].astype(BF16)
        filt[:, at] = y.astype(F32)
        for m in range(4):
            sums[m, :, at] = product(y, diag[m, at, :])

    lanes = min(512, width)
    groups = length // 8
    place = lax.broadcasted_iota(jnp.int32, (8, lanes), 0)

    for lane in range(0, width, lanes):
        at = pl.ds(lane, lanes)
        rates = -FADING_FACTOR * small_softplus(odds_ref[:, at])

        def step(i, carry):
            result = []
            for d in range(2):
                group = i if d == 0 else groups - 1 - i
                here = pl.ds(pl.multiple_of(group * 8, 8), 8)
                cols = cols_ref[here, :]
                log_keep = cols[:, d : d + 1] * sigmoid(sums[2 * d, here, at]) * rates[d : d + 1]
                log_keep = log_keep + cols[:, 2 + d : 3 + d]
                a = jnp.exp(log_keep)
                root = jnp.sqrt(one_less_exp(2.0 * log_keep, a * a))
                b = root * sigmoid(sums[2 * d + 1, here, at]) * filt[here, at]
                for k in (1, 2, 4):
                    if d == 0:
                        inside, shift = place >= k, k
                    else:
                        inside, shift = place < 8 - k, 8 - k
                    b = jnp.where(inside, b + a * pltpu.roll(b, shift, 0), b)
                    a = jnp.where(inside, a * pltpu.roll(a, shift, 0), a)
                kept, state = carry[2 * d], carry[2 * d + 1]
                b = b + a * state
                a = a * kept
                keep[d, here, at] = a
                loc[d, here, at] = b
                last = 7 if d == 0 else 0
                result += [a[last : last + 1], b[last : last + 1]]
            return tuple(result)

        one, zero = jnp.ones((1, lanes), F32), jnp.zeros((1, lanes), F32)
        ends = lax.fori_loop(0, groups, step, (one, zero, one, zero), unroll=2)
        for d in range(2):
            summary[d, 0:1, at] = ends[2 * d]
            summary[d, 1:2, at] = ends[2 * d + 1]

    carries = []
    for k in range(1, n_sp):
        to = lax.rem(sp + k, n_sp)
        way = jnp.where(to > sp, 0, 1)
        copy = pltpu.make_async_remote_copy(
            src_ref=summary.at[way],
            dst_ref=totals.at[k],
            send_sem=c_send.at[k],
            recv_sem=c_recv.at[k],
            device_id=(to, tp),
            device_id_type=MESH,
        )
        copy.start()
        carries.append(copy)

    project(wg, g_buf, tile, rows, far, pieces, gelu)
    project(wp, p_buf, ptile, rows, far + 2 * EDGE, pieces + edges, same)
    gw = cluster_ref.shape[1]
    local_groups = pool_width // gw
    position = sp * length + lax.broadcasted_iota(jnp.int32, (length, gw), 0)
    total_length = length * n_sp
    for j in range(local_groups):
        x = p_buf[:, j * gw : (j + 1) * gw]
        level = x
        code_here = lax.rem(tp * local_groups + j, 4)
        codes = (j % 4,) if local_groups % 4 == 0 else range(4)
        pooled = None
        for code in range(codes[-1] + 1):
            h = 1 << code
            level = level + pltpu.roll(level, total_rows - h, 0)
            if code not in codes:
                continue
            window = pltpu.roll(level, h, 0)[EDGE : EDGE + length]
            counted = jnp.minimum(position + h, total_length) - jnp.maximum(position - h, 0)
            value = window / counted.astype(F32)
            pooled = value if pooled is None else jnp.where(code_here == code, value, pooled)
        pooled = (pooled - x[EDGE : EDGE + length]).astype(BF16)
        mapped = product(pooled, cluster_ref[j]) * factor_ref[:, j * gw : (j + 1) * gw].astype(F32)
        pool_mix[:, j * gw : (j + 1) * gw] = mapped.astype(BF16)

    for copy in carries:
        copy.wait_recv()
    forward = jnp.zeros((1, width), F32)
    backward = jnp.zeros((1, width), F32)
    for k in range(n_sp - 1, 0, -1):
        valid = k <= sp
        forward = jnp.where(valid, totals[k, 0:1, :] * forward + totals[k, 1:2, :], forward)
    for k in range(1, n_sp):
        valid = k > sp
        backward = jnp.where(valid, totals[k, 0:1, :] * backward + totals[k, 1:2, :], backward)

    loads[4].wait()
    loads[5].wait()
    columns = wso.shape[1]
    parts = part.shape[1]
    ctile = columns // parts

    def mix_rows(first):
        @pl.loop(0, rows // 16)
        def _(i):
            here = pl.ds(pl.multiple_of(first + i * 16, 16), 16)
            state = loc[0, here, :] + keep[0, here, :] * forward
            state = state + loc[1, here, :] + keep[1, here, :] * backward
            gate = g_buf[pl.ds(pl.multiple_of(EDGE + first + i * 16, 16), 16), :]
            mix[here, :] = (gate * state).astype(BF16)

    def share(first, c):
        here = pl.ds(first, rows)
        at = pl.ds(c * ctile, ctile)
        return product(mix[here, :], wso[:, at]) + product(pool_mix[here, :], wpo[:, at])

    scatters = []
    for k in range(1, n_tp):
        to = lax.rem(tp + k, n_tp)
        first = pl.multiple_of(to * rows, 16)
        mix_rows(first)
        for c in range(parts):
            part[k - 1, c] = share(first, c).astype(BF16)
            scatters.append(
                pltpu.make_async_remote_copy(
                    src_ref=part.at[k - 1, c],
                    dst_ref=landed.at[k - 1, c],
                    send_sem=rs_send.at[k - 1, c],
                    recv_sem=rs_recv.at[k - 1, c],
                    device_id=(sp, to),
                    device_id_type=MESH,
                )
            )
            if len(scatters) > 1:
                scatters[-2].start()
    first = pl.multiple_of(tp * rows, 16)
    mix_rows(first)
    if scatters:
        scatters[-1].start()
    for c in range(parts):
        x_total = share(first, c)
        for k in range(1, n_tp):
            scatters[(k - 1) * parts + c].wait_recv()
            x_total = x_total + landed[k - 1, c].astype(F32)
        out_ref[:, c * ctile : (c + 1) * ctile] = x_total.astype(BF16)

    for copy in gathers + carries + scatters:
        copy.wait_send()
    for side, sender in ((0, n_tp - 1), (1, 0)):

        @pl.when(tp == sender)
        def _():
            for j in range(n_tp):
                halo_copy(side, j, j).wait_send()


def local(
    n_sp,
    n_tp,
    incoming_activity,
    entry_standardize_factor,
    recursive_entry_matrix,
    final_switch_matrix,
    averaging_entry_matrix,
    percolumn_filter_coefficients,
    switch_tiled_matrices,
    prior_fading_odds,
    speed_factors,
    extra_fading_amounts,
    averaging_cluster_matrices,
    averaging_feature_factor,
    recursive_final_matrix,
    averaging_final_matrix,
):
    rows, depth = incoming_activity.shape
    length = rows * n_tp
    width = recursive_entry_matrix.shape[1]
    pool_width = averaging_entry_matrix.shape[1]
    columns = recursive_final_matrix.shape[1]
    half = switch_tiled_matrices.shape[-1]
    cols = jnp.transpose(jnp.concatenate([speed_factors, extra_fading_amounts], axis=0))
    parts = 4
    tile = min(256, width)
    hbm = pl.BlockSpec(memory_space=pl.ANY)
    vmem = pl.BlockSpec(memory_space=pltpu.VMEM)
    dma = pltpu.SemaphoreType.DMA
    peers = max(n_tp - 1, 1)
    padded = length + 2 * EDGE
    return pl.pallas_call(
        functools.partial(kernel, n_sp, n_tp),
        out_shape=jax.ShapeDtypeStruct((rows, columns), BF16),
        in_specs=[hbm, vmem, hbm, hbm, hbm, vmem, vmem, vmem, vmem, vmem, vmem, hbm, hbm],
        out_specs=vmem,
        scratch_shapes=[
            pltpu.VMEM((rows, depth), BF16),
            pltpu.VMEM((rows * peers, depth), BF16),
            pltpu.VMEM((2, EDGE, depth), BF16),
            pltpu.VMEM((padded, depth), BF16),
            pltpu.VMEM((depth, width), BF16),
            pltpu.VMEM((depth, width), BF16),
            pltpu.VMEM((depth, pool_width), BF16),
            pltpu.VMEM((width, columns), BF16),
            pltpu.VMEM((pool_width, columns), BF16),
            pltpu.VMEM((padded, width), F32),
            pltpu.VMEM((padded, width), F32),
            pltpu.VMEM((padded, pool_width), F32),
            pltpu.VMEM((length, width), F32),
            pltpu.VMEM((4, width, tile), BF16),
            pltpu.VMEM((4, length, width), F32),
            pltpu.VMEM((2, length, width), F32),
            pltpu.VMEM((2, length, width), F32),
            pltpu.VMEM((2, 2, width), F32),
            pltpu.VMEM((n_sp, 2, width), F32),
            pltpu.VMEM((length, width), BF16),
            pltpu.VMEM((length, pool_width), BF16),
            pltpu.VMEM((peers, parts, rows, columns // parts), BF16),
            pltpu.VMEM((peers, parts, rows, columns // parts), BF16),
            dma((6,)),
            dma((n_tp,)),
            dma((n_tp,)),
            dma((2, n_tp)),
            dma((2,)),
            dma((n_sp,)),
            dma((n_sp,)),
            dma((peers, parts)),
            dma((peers, parts)),
        ],
        compiler_params=pltpu.CompilerParams(
            has_side_effects=True, vmem_limit_bytes=63 * 1024 * 1024
        ),
    )(
        incoming_activity,
        entry_standardize_factor.reshape(1, depth),
        recursive_entry_matrix,
        final_switch_matrix,
        averaging_entry_matrix,
        percolumn_filter_coefficients,
        switch_tiled_matrices.reshape(4, width, half),
        prior_fading_odds,
        cols,
        averaging_cluster_matrices,
        averaging_feature_factor.reshape(1, pool_width),
        recursive_final_matrix,
        averaging_final_matrix,
    )


def solution(mesh):
    in_specs = (
        P(("sp", "tp"), None),
        P(),
        P(None, "tp"),
        P(None, "tp"),
        P(None, "tp"),
        P(None, "tp"),
        P(None, None, "tp", None, None),
        P(None, "tp"),
        P(None, "sp"),
        P(None, "sp"),
        P("tp", None, None),
        P("tp"),
        P("tp", None),
        P("tp", None),
    )
    out_specs = P(("sp", "tp"), None)
    body = functools.partial(local, mesh.shape["sp"], mesh.shape["tp"])
    return jax.shard_map(body, mesh=mesh, in_specs=in_specs, out_specs=out_specs, check_vma=False)
```

```python
import functools

import jax
import jax.numpy as jnp
from jax import lax
from jax.experimental import pallas as pl
from jax.experimental.pallas import tpu as pltpu
from jax.sharding import PartitionSpec as P

FADING_FACTOR = 8.0
epsilon = 1e-06
EDGE = 16
MESH = pl.DeviceIdType.MESH
F32 = jnp.float32
BF16 = jnp.bfloat16


def product(left, right):
    return jnp.dot(left, right, preferred_element_type=F32)


def small_softplus(odds):
    e = jnp.exp(-odds)
    z = e / (2.0 + e)
    y = z * z
    return 2.0 * z * (1.0 + y * (1.0 / 3.0 + y * (1.0 / 5.0 + y * (1.0 / 7.0))))


def minus_tanh(u):
    near = -u * (1.0 - u * u * (1.0 / 3.0))
    return jnp.where(u > -0.015625, near, jnp.tanh(-u))


def kernel(
    n_sp,
    n_tp,
    x_hbm,
    gain_ref,
    ws_hbm,
    wg_hbm,
    wp_hbm,
    conv_ref,
    switch_ref,
    odds_ref,
    speed_ref,
    extra_ref,
    cluster_ref,
    factor_ref,
    wso_hbm,
    wpo_hbm,
    out_ref,
    x_own,
    x_far,
    halo,
    near,
    cols,
    normed,
    ws,
    wg,
    wp,
    wso,
    wpo,
    s_buf,
    g_buf,
    p_buf,
    filt,
    diag,
    sums,
    keep,
    loc,
    ends_buf,
    carry_in,
    summary,
    totals,
    mix,
    pool_mix,
    part,
    landed,
    w_sem,
    ag_send,
    ag_recv,
    halo_send,
    halo_recv,
    near_send,
    near_recv,
    c_send,
    c_recv,
    rs_send,
    rs_recv,
):
    sp = lax.axis_index("sp")
    tp = lax.axis_index("tp")
    rows, depth = x_own.shape
    length = rows * n_tp
    width = ws.shape[1]
    pool_width = wp.shape[1]

    gathers = []
    nxt = lax.rem(sp + 1, n_sp)
    prv = lax.rem(sp + n_sp - 1, n_sp)

    def halo_copy(side, tp_to, slot):
        src = x_hbm.at[pl.ds(rows - EDGE if side == 0 else 0, EDGE)]
        return pltpu.make_async_remote_copy(
            src_ref=src,
            dst_ref=halo.at[side],
            send_sem=halo_send.at[side, slot],
            recv_sem=halo_recv.at[side],
            device_id=(nxt if side == 0 else prv, tp_to),
            device_id_type=MESH,
        )

    for side, sender in ((0, n_tp - 1), (1, 0)):

        @pl.when(tp == sender)
        def _():
            for j in range(n_tp):
                halo_copy(side, j, j).start()

    up_tp = lax.rem(tp + 1, n_tp)
    down_tp = lax.rem(tp + n_tp - 1, n_tp)
    up = (jnp.where(tp == n_tp - 1, nxt, sp), up_tp)
    down = (jnp.where(tp == 0, prv, sp), down_tp)
    nears = []
    for side, to in ((0, up), (1, down)):
        copy = pltpu.make_async_remote_copy(
            src_ref=x_hbm.at[pl.ds(rows - EDGE if side == 0 else 0, EDGE)],
            dst_ref=near.at[side],
            send_sem=near_send.at[side],
            recv_sem=near_recv.at[side],
            device_id=to,
            device_id_type=MESH,
        )
        copy.start()
        nears.append(copy)
    pieces_in = ag_send.shape[1]
    piece = rows // pieces_in
    for k in range(1, n_tp):
        for q in range(pieces_in):
            copy = pltpu.make_async_remote_copy(
                src_ref=x_hbm.at[pl.ds(q * piece, piece)],
                dst_ref=x_far.at[pl.ds((k - 1) * rows + q * piece, piece)],
                send_sem=ag_send.at[k, q],
                recv_sem=ag_recv.at[k, q],
                device_id=(sp, lax.rem(tp + k, n_tp)),
                device_id_type=MESH,
            )
            copy.start()
            gathers.append(copy)
    loads = []
    for i, (src, dst) in enumerate(
        (
            (x_hbm, x_own),
            (ws_hbm, ws),
            (wg_hbm, wg),
            (wp_hbm, wp),
            (wso_hbm, wso),
            (wpo_hbm, wpo),
        )
    ):
        copy = pltpu.make_async_copy(src, dst, w_sem.at[i])
        copy.start()
        loads.append(copy)

    gain = gain_ref[...].astype(F32).reshape(1, depth)
    fill = jnp.zeros((6, length), F32)
    cols[...] = jnp.transpose(jnp.concatenate([extra_ref[...], fill], axis=0))

    def normalise(src, count, at, begin=0):
        @pl.loop(0, count // 16)
        def _(i):
            at_row = pl.multiple_of(i * 16, 16)
            values = src[pl.ds(pl.multiple_of(begin + at_row, 16), 16), :].astype(F32)
            mean = jnp.mean(values * values, axis=1, keepdims=True)
            scaled = values * lax.rsqrt(mean + epsilon)
            normed[pl.ds(pl.multiple_of(at + at_row, 16), 16), :] = (scaled * gain).astype(BF16)

    tile = min(256, width)
    ptile = min(256, pool_width)

    def owner_row(k):
        return pl.multiple_of(EDGE + lax.rem(tp + n_tp - k, n_tp) * rows, 16)

    def project(weights, buf, step, first, count, pieces, act):
        @pl.loop(0, weights.shape[1] // step)
        def _(c):
            at = pl.ds(pl.multiple_of(c * step, step), step)
            value = product(normed[pl.ds(first, count), :], weights[:, at]).astype(BF16)
            value = act(value.astype(F32))
            for begin, size, row in pieces:
                buf[pl.ds(row, size), at] = value[begin : begin + size]

    same = lambda v: v
    gelu = functools.partial(jax.nn.gelu, approximate=True)

    half = switch_ref.shape[2]
    spread = (
        lax.broadcasted_iota(jnp.int32, (half, tile), 1) % half
        == lax.broadcasted_iota(jnp.int32, (half, tile), 0)
    ).astype(F32).astype(BF16)
    on_diag = (
        lax.broadcasted_iota(jnp.int32, (tile, tile), 0) // half
        == lax.broadcasted_iota(jnp.int32, (tile, tile), 1) // half
    )
    for m in range(4):

        @pl.loop(0, width // tile)
        def _(g):
            at = pl.ds(pl.multiple_of(g * tile, tile), tile)
            wide = product(switch_ref[m, at, :], spread)
            diag[m, at, :] = jnp.where(on_diag, 0.5 * wide, 0.0).astype(BF16)

    lanes = min(512, width)
    groups = rows // 8
    place = lax.broadcasted_iota(jnp.int32, (8, lanes), 0)
    window = rows + 2 * EDGE

    def chunk(owner):
        base = pl.multiple_of(owner * rows, 16)

        @pl.loop(0, width // tile)
        def _(g):
            at = pl.ds(pl.multiple_of(g * tile, tile), tile)
            taps = conv_ref[:, at].astype(F32)
            x = s_buf[pl.ds(base, window), at]
            y = taps[0:1] * pltpu.roll(x, 2, 0)
            y = y + taps[1:2] * pltpu.roll(x, 1, 0)
            y = y + taps[2:3] * x
            y = y + taps[3:4] * pltpu.roll(x, window - 1, 0)
            y = y[EDGE : EDGE + rows].astype(BF16)
            filt[:, at] = 0.5 * y.astype(F32)
            for m in range(4):
                sums[m, :, at] = product(y, diag[m, at, :])

        for lane in range(0, width, lanes):
            at = pl.ds(lane, lanes)
            rates = -0.5 * FADING_FACTOR * small_softplus(odds_ref[:, at]) * speed_ref[:, 0:1]

            def step(i, carry):
                result = []
                for d in range(2):
                    group = i if d == 0 else groups - 1 - i
                    here = pl.ds(pl.multiple_of(group * 8, 8), 8)
                    there = pl.ds(pl.multiple_of(base + group * 8, 8), 8)
                    rate = rates[d : d + 1]
                    log_keep = jnp.tanh(sums[2 * d, here, at]) * rate + rate
                    log_keep = log_keep + cols[there, d : d + 1]
                    a = jnp.exp(log_keep)
                    square = minus_tanh(log_keep) * (1.0 + a * a)
                    root = square * lax.rsqrt(square + 1e-37)
                    f = filt[here, at]
                    b = root * (f + f * jnp.tanh(sums[2 * d + 1, here, at]))
                    for k in (1, 2, 4):
                        if d == 0:
                            inside, shift = place >= k, k
                        else:
                            inside, shift = place < 8 - k, 8 - k
                        b = jnp.where(inside, b + a * pltpu.roll(b, shift, 0), b)
                        a = jnp.where(inside, a * pltpu.roll(a, shift, 0), a)
                    kept, state = carry[2 * d], carry[2 * d + 1]
                    b = b + a * state
                    a = a * kept
                    keep[d, there, at] = a
                    loc[d, there, at] = b
                    last = 7 if d == 0 else 0
                    result += [a[last : last + 1], b[last : last + 1]]
                return tuple(result)

            one, zero = jnp.ones((1, lanes), F32), jnp.zeros((1, lanes), F32)
            ends = lax.fori_loop(0, groups, step, (one, zero, one, zero), unroll=2)
            for m in range(4):
                ends_buf[owner, m : m + 1, at] = ends[m]

    far = rows * (n_tp - 1)
    total_rows = length + 2 * EDGE
    edge_at = rows + far
    loads[0].wait()
    normalise(x_own, rows, 0)
    for copy in nears:
        copy.wait_recv()
    for side in range(2):
        normalise(near.at[side], EDGE, rows + side * EDGE)

    @pl.when(jnp.logical_and(sp == 0, tp == 0))
    def _():
        normed[pl.ds(rows, EDGE), :] = jnp.zeros((EDGE, depth), BF16)

    @pl.when(jnp.logical_and(sp == n_sp - 1, tp == n_tp - 1))
    def _():
        normed[pl.ds(rows + EDGE, EDGE), :] = jnp.zeros((EDGE, depth), BF16)

    own = ((0, rows, owner_row(0)),)
    own_edges = (
        (rows, EDGE, pl.multiple_of(tp * rows, 16)),
        (rows + EDGE, EDGE, pl.multiple_of(EDGE + tp * rows + rows, 16)),
    )
    loads[1].wait()
    project(ws, s_buf, tile, 0, rows + 2 * EDGE, own + own_edges, same)
    chunk(tp)
    loads[2].wait()
    project(wg, g_buf, tile, 0, rows, own, gelu)
    loads[3].wait()
    project(wp, p_buf, ptile, 0, rows, own, same)

    for side in range(2):
        halo_copy(side, 0, 0).wait_recv()
        normalise(halo.at[side], EDGE, edge_at + side * EDGE)

    @pl.when(sp == 0)
    def _():
        normed[pl.ds(edge_at, EDGE), :] = jnp.zeros((EDGE, depth), BF16)

    @pl.when(sp == n_sp - 1)
    def _():
        normed[pl.ds(edge_at + EDGE, EDGE), :] = jnp.zeros((EDGE, depth), BF16)

    for n, copy in enumerate(gathers):
        copy.wait_recv()
        normalise(x_far, piece, rows + n * piece, n * piece)
    pieces = [((k - 1) * rows, rows, owner_row(k)) for k in range(1, n_tp)]
    edges = [(far, EDGE, 0), (far + EDGE, EDGE, EDGE + length)]
    project(ws, s_buf, tile, rows, far + 2 * EDGE, pieces + edges, same)
    for k in range(1, n_tp):
        chunk(lax.rem(tp + n_tp - k, n_tp))

    for d in range(2):
        kept, state = jnp.ones((1, width), F32), jnp.zeros((1, width), F32)
        for j in range(n_tp) if d == 0 else range(n_tp - 1, -1, -1):
            step_keep = ends_buf[j, 2 * d : 2 * d + 1, :]
            state = step_keep * state + ends_buf[j, 2 * d + 1 : 2 * d + 2, :]
            kept = step_keep * kept
        summary[d, 0:1, :] = kept
        summary[d, 1:2, :] = state

    carries = []
    for k in range(1, n_sp):
        to = lax.rem(sp + k, n_sp)
        way = jnp.where(to > sp, 0, 1)
        copy = pltpu.make_async_remote_copy(
            src_ref=summary.at[way],
            dst_ref=totals.at[k],
            send_sem=c_send.at[k],
            recv_sem=c_recv.at[k],
            device_id=(to, tp),
            device_id_type=MESH,
        )
        copy.start()
        carries.append(copy)

    project(wg, g_buf, tile, rows, far, pieces, gelu)
    project(wp, p_buf, ptile, rows, far + 2 * EDGE, pieces + edges, same)
    gw = cluster_ref.shape[1]
    local_groups = pool_width // gw
    factors = factor_ref[...].astype(F32).reshape(1, pool_width)
    position = sp * length + lax.broadcasted_iota(jnp.int32, (length, gw), 0)
    total_length = length * n_sp
    for j in range(local_groups):
        x = p_buf[:, j * gw : (j + 1) * gw]
        level = x
        code_here = lax.rem(tp * local_groups + j, 4)
        codes = (j % 4,) if local_groups % 4 == 0 else range(4)
        pooled = None
        for code in range(codes[-1] + 1):
            h = 1 << code
            level = level + pltpu.roll(level, total_rows - h, 0)
            if code not in codes:
                continue
            spanned = pltpu.roll(level, h, 0)[EDGE : EDGE + length]
            counted = jnp.minimum(position + h, total_length) - jnp.maximum(position - h, 0)
            value = spanned / counted.astype(F32)
            pooled = value if pooled is None else jnp.where(code_here == code, value, pooled)
        pooled = (pooled - x[EDGE : EDGE + length]).astype(BF16)
        mapped = product(pooled, cluster_ref[j]) * factors[:, j * gw : (j + 1) * gw]
        pool_mix[:, j * gw : (j + 1) * gw] = mapped.astype(BF16)

    for copy in carries:
        copy.wait_recv()
    forward = jnp.zeros((1, width), F32)
    backward = jnp.zeros((1, width), F32)
    for k in range(n_sp - 1, 0, -1):
        valid = k <= sp
        forward = jnp.where(valid, totals[k, 0:1, :] * forward + totals[k, 1:2, :], forward)
    for k in range(1, n_sp):
        valid = k > sp
        backward = jnp.where(valid, totals[k, 0:1, :] * backward + totals[k, 1:2, :], backward)

    for j in range(n_tp):
        carry_in[j, 0:1, :] = forward
        forward = ends_buf[j, 0:1, :] * forward + ends_buf[j, 1:2, :]
    for j in range(n_tp - 1, -1, -1):
        carry_in[j, 1:2, :] = backward
        backward = ends_buf[j, 2:3, :] * backward + ends_buf[j, 3:4, :]

    loads[4].wait()
    loads[5].wait()
    columns = wso.shape[1]
    parts = part.shape[1]
    ctile = columns // parts

    def mix_rows(owner):
        first = owner * rows
        forward = carry_in[owner, 0:1, :]
        backward = carry_in[owner, 1:2, :]

        @pl.loop(0, rows // 16)
        def _(i):
            here = pl.ds(pl.multiple_of(first + i * 16, 16), 16)
            state = loc[0, here, :] + keep[0, here, :] * forward
            state = state + loc[1, here, :] + keep[1, here, :] * backward
            gate = g_buf[pl.ds(pl.multiple_of(EDGE + first + i * 16, 16), 16), :]
            mix[here, :] = (gate * state).astype(BF16)

    def share(first, c):
        here = pl.ds(first, rows)
        at = pl.ds(c * ctile, ctile)
        return product(mix[here, :], wso[:, at]) + product(pool_mix[here, :], wpo[:, at])

    scatters = []
    for k in range(1, n_tp):
        to = lax.rem(tp + k, n_tp)
        first = pl.multiple_of(to * rows, 16)
        mix_rows(to)
        for c in range(parts):
            part[k - 1, c] = share(first, c).astype(BF16)
            scatters.append(
                pltpu.make_async_remote_copy(
                    src_ref=part.at[k - 1, c],
                    dst_ref=landed.at[k - 1, c],
                    send_sem=rs_send.at[k - 1, c],
                    recv_sem=rs_recv.at[k - 1, c],
                    device_id=(sp, to),
                    device_id_type=MESH,
                )
            )
            if len(scatters) > 1:
                scatters[-2].start()
    first = pl.multiple_of(tp * rows, 16)
    mix_rows(tp)
    if scatters:
        scatters[-1].start()
    for c in range(parts):
        x_total = share(first, c)
        for k in range(1, n_tp):
            scatters[(k - 1) * parts + c].wait_recv()
            x_total = x_total + landed[k - 1, c].astype(F32)
        out_ref[:, c * ctile : (c + 1) * ctile] = x_total.astype(BF16)

    for copy in gathers + nears + carries + scatters:
        copy.wait_send()
    for side, sender in ((0, n_tp - 1), (1, 0)):

        @pl.when(tp == sender)
        def _():
            for j in range(n_tp):
                halo_copy(side, j, j).wait_send()


def local(
    n_sp,
    n_tp,
    incoming_activity,
    entry_standardize_factor,
    recursive_entry_matrix,
    final_switch_matrix,
    averaging_entry_matrix,
    percolumn_filter_coefficients,
    switch_tiled_matrices,
    prior_fading_odds,
    speed_factors,
    extra_fading_amounts,
    averaging_cluster_matrices,
    averaging_feature_factor,
    recursive_final_matrix,
    averaging_final_matrix,
):
    rows, depth = incoming_activity.shape
    length = rows * n_tp
    width = recursive_entry_matrix.shape[1]
    pool_width = averaging_entry_matrix.shape[1]
    columns = recursive_final_matrix.shape[1]
    half = switch_tiled_matrices.shape[-1]
    parts = 4
    tile = min(256, width)
    hbm = pl.BlockSpec(memory_space=pl.ANY)
    vmem = pl.BlockSpec(memory_space=pltpu.VMEM)
    dma = pltpu.SemaphoreType.DMA
    peers = max(n_tp - 1, 1)
    padded = length + 2 * EDGE
    return pl.pallas_call(
        functools.partial(kernel, n_sp, n_tp),
        out_shape=jax.ShapeDtypeStruct((rows, columns), BF16),
        in_specs=[hbm, vmem, hbm, hbm, hbm, vmem, vmem, vmem, vmem, vmem, vmem, vmem, hbm, hbm],
        out_specs=vmem,
        scratch_shapes=[
            pltpu.VMEM((rows, depth), BF16),
            pltpu.VMEM((rows * peers, depth), BF16),
            pltpu.VMEM((2, EDGE, depth), BF16),
            pltpu.VMEM((2, EDGE, depth), BF16),
            pltpu.VMEM((length, 8), F32),
            pltpu.VMEM((padded, depth), BF16),
            pltpu.VMEM((depth, width), BF16),
            pltpu.VMEM((depth, width), BF16),
            pltpu.VMEM((depth, pool_width), BF16),
            pltpu.VMEM((width, columns), BF16),
            pltpu.VMEM((pool_width, columns), BF16),
            pltpu.VMEM((padded, width), F32),
            pltpu.VMEM((padded, width), F32),
            pltpu.VMEM((padded, pool_width), F32),
            pltpu.VMEM((rows, width), F32),
            pltpu.VMEM((4, width, tile), BF16),
            pltpu.VMEM((4, rows, width), F32),
            pltpu.VMEM((2, length, width), F32),
            pltpu.VMEM((2, length, width), F32),
            pltpu.VMEM((n_tp, 4, width), F32),
            pltpu.VMEM((n_tp, 2, width), F32),
            pltpu.VMEM((2, 2, width), F32),
            pltpu.VMEM((n_sp, 2, width), F32),
            pltpu.VMEM((length, width), BF16),
            pltpu.VMEM((length, pool_width), BF16),
            pltpu.VMEM((peers, parts, rows, columns // parts), BF16),
            pltpu.VMEM((peers, parts, rows, columns // parts), BF16),
            dma((6,)),
            dma((n_tp, 4)),
            dma((n_tp, 4)),
            dma((2, n_tp)),
            dma((2,)),
            dma((2,)),
            dma((2,)),
            dma((n_sp,)),
            dma((n_sp,)),
            dma((peers, parts)),
            dma((peers, parts)),
        ],
        compiler_params=pltpu.CompilerParams(
            has_side_effects=True, vmem_limit_bytes=63 * 1024 * 1024
        ),
    )(
        incoming_activity,
        entry_standardize_factor,
        recursive_entry_matrix,
        final_switch_matrix,
        averaging_entry_matrix,
        percolumn_filter_coefficients,
        switch_tiled_matrices.reshape(4, width, half),
        prior_fading_odds,
        speed_factors,
        extra_fading_amounts,
        averaging_cluster_matrices,
        averaging_feature_factor,
        recursive_final_matrix,
        averaging_final_matrix,
    )


def solution(mesh):
    in_specs = (
        P(("sp", "tp"), None),
        P(),
        P(None, "tp"),
        P(None, "tp"),
        P(None, "tp"),
        P(None, "tp"),
        P(None, None, "tp", None, None),
        P(None, "tp"),
        P(None, "sp"),
        P(None, "sp"),
        P("tp", None, None),
        P("tp"),
        P("tp", None),
        P("tp", None),
    )
    out_specs = P(("sp", "tp"), None)
    body = functools.partial(local, mesh.shape["sp"], mesh.shape["tp"])
    return jax.shard_map(body, mesh=mesh, in_specs=in_specs, out_specs=out_specs, check_vma=False)
```

```python
import functools

import jax
import jax.numpy as jnp
from jax import lax
from jax.experimental import pallas as pl
from jax.experimental.pallas import tpu as pltpu
from jax.sharding import PartitionSpec as P

FADING_FACTOR = 8.0
epsilon = 1e-06
EDGE = 16
MESH = pl.DeviceIdType.MESH
F32 = jnp.float32
BF16 = jnp.bfloat16


def product(left, right):
    return jnp.dot(left, right, preferred_element_type=F32)


def small_softplus(odds):
    e = jnp.exp(-odds)
    z = e / (2.0 + e)
    y = z * z
    return 2.0 * z * (1.0 + y * (1.0 / 3.0 + y * (1.0 / 5.0 + y * (1.0 / 7.0))))


def minus_tanh(u):
    near = -u * (1.0 - u * u * (1.0 / 3.0))
    return jnp.where(u > -0.015625, near, jnp.tanh(-u))


def kernel(
    n_sp,
    n_tp,
    x_hbm,
    gain_ref,
    ws_hbm,
    wg_hbm,
    wp_hbm,
    conv_ref,
    switch_ref,
    odds_ref,
    speed_ref,
    extra_ref,
    cluster_ref,
    factor_ref,
    wso_hbm,
    wpo_hbm,
    out_ref,
    x_own,
    x_far,
    halo,
    near,
    cols,
    normed,
    ws,
    wg,
    wp,
    wso,
    wpo,
    s_buf,
    g_buf,
    p_buf,
    filt,
    diag,
    sums,
    keep,
    loc,
    ends_buf,
    carry_in,
    summary,
    totals,
    mix,
    pool_mix,
    part,
    landed,
    w_sem,
    ag_send,
    ag_recv,
    halo_send,
    halo_recv,
    near_send,
    near_recv,
    c_send,
    c_recv,
    rs_send,
    rs_recv,
):
    sp = lax.axis_index("sp")
    tp = lax.axis_index("tp")
    rows, depth = x_own.shape
    length = rows * n_tp
    width = ws.shape[1]
    pool_width = wp.shape[1]

    gathers = []
    nxt = lax.rem(sp + 1, n_sp)
    prv = lax.rem(sp + n_sp - 1, n_sp)

    def halo_copy(side, tp_to, slot):
        src = x_hbm.at[pl.ds(rows - EDGE if side == 0 else 0, EDGE)]
        return pltpu.make_async_remote_copy(
            src_ref=src,
            dst_ref=halo.at[side],
            send_sem=halo_send.at[side, slot],
            recv_sem=halo_recv.at[side],
            device_id=(nxt if side == 0 else prv, tp_to),
            device_id_type=MESH,
        )

    for side, sender in ((0, n_tp - 1), (1, 0)):

        @pl.when(tp == sender)
        def _():
            for j in range(n_tp):
                halo_copy(side, j, j).start()

    up_tp = lax.rem(tp + 1, n_tp)
    down_tp = lax.rem(tp + n_tp - 1, n_tp)
    up = (jnp.where(tp == n_tp - 1, nxt, sp), up_tp)
    down = (jnp.where(tp == 0, prv, sp), down_tp)
    nears = []
    for side, to in ((0, up), (1, down)):
        copy = pltpu.make_async_remote_copy(
            src_ref=x_hbm.at[pl.ds(rows - EDGE if side == 0 else 0, EDGE)],
            dst_ref=near.at[side],
            send_sem=near_send.at[side],
            recv_sem=near_recv.at[side],
            device_id=to,
            device_id_type=MESH,
        )
        copy.start()
        nears.append(copy)
    pieces_in = ag_send.shape[1]
    piece = rows // pieces_in
    for k in range(1, n_tp):
        for q in range(pieces_in):
            copy = pltpu.make_async_remote_copy(
                src_ref=x_hbm.at[pl.ds(q * piece, piece)],
                dst_ref=x_far.at[pl.ds((k - 1) * rows + q * piece, piece)],
                send_sem=ag_send.at[k, q],
                recv_sem=ag_recv.at[k, q],
                device_id=(sp, lax.rem(tp + k, n_tp)),
                device_id_type=MESH,
            )
            copy.start()
            gathers.append(copy)
    loads = []
    for i, (src, dst) in enumerate(
        (
            (x_hbm, x_own),
            (ws_hbm, ws),
            (wg_hbm, wg),
            (wp_hbm, wp),
            (wso_hbm, wso),
            (wpo_hbm, wpo),
        )
    ):
        copy = pltpu.make_async_copy(src, dst, w_sem.at[i])
        copy.start()
        loads.append(copy)

    gain = gain_ref[...].astype(F32).reshape(1, depth)
    fill = jnp.zeros((6, length), F32)
    cols[...] = jnp.transpose(jnp.concatenate([extra_ref[...], fill], axis=0))

    def normalise(src, count, at, begin=0):
        @pl.loop(0, count // 16)
        def _(i):
            at_row = pl.multiple_of(i * 16, 16)
            values = src[pl.ds(pl.multiple_of(begin + at_row, 16), 16), :].astype(F32)
            mean = jnp.mean(values * values, axis=1, keepdims=True)
            scaled = values * lax.rsqrt(mean + epsilon)
            normed[pl.ds(pl.multiple_of(at + at_row, 16), 16), :] = (scaled * gain).astype(BF16)

    tile = min(256, width)
    ptile = min(256, pool_width)

    def owner_row(k):
        return pl.multiple_of(EDGE + lax.rem(tp + n_tp - k, n_tp) * rows, 16)

    def project(weights, buf, step, first, count, pieces, act):
        @pl.loop(0, weights.shape[1] // step)
        def _(c):
            at = pl.ds(pl.multiple_of(c * step, step), step)
            value = product(normed[pl.ds(first, count), :], weights[:, at]).astype(BF16)
            value = act(value.astype(F32))
            for begin, size, row in pieces:
                buf[pl.ds(row, size), at] = value[begin : begin + size]

    same = lambda v: v
    gelu = functools.partial(jax.nn.gelu, approximate=True)

    half = switch_ref.shape[2]
    spread = (
        lax.broadcasted_iota(jnp.int32, (half, tile), 1) % half
        == lax.broadcasted_iota(jnp.int32, (half, tile), 0)
    ).astype(F32).astype(BF16)
    on_diag = (
        lax.broadcasted_iota(jnp.int32, (tile, tile), 0) // half
        == lax.broadcasted_iota(jnp.int32, (tile, tile), 1) // half
    )
    for m in range(4):

        @pl.loop(0, width // tile)
        def _(g):
            at = pl.ds(pl.multiple_of(g * tile, tile), tile)
            wide = product(switch_ref[m, at, :], spread)
            diag[m, at, :] = jnp.where(on_diag, 0.5 * wide, 0.0).astype(BF16)

    lanes = min(512, width)
    groups = rows // 8
    place = lax.broadcasted_iota(jnp.int32, (8, lanes), 0)
    window = rows + 2 * EDGE

    def chunk(owner):
        base = pl.multiple_of(owner * rows, 16)

        @pl.loop(0, width // tile)
        def _(g):
            at = pl.ds(pl.multiple_of(g * tile, tile), tile)
            taps = conv_ref[:, at].astype(F32)
            x = s_buf[pl.ds(base, window), at]
            y = taps[0:1] * pltpu.roll(x, 2, 0)
            y = y + taps[1:2] * pltpu.roll(x, 1, 0)
            y = y + taps[2:3] * x
            y = y + taps[3:4] * pltpu.roll(x, window - 1, 0)
            y = y[EDGE : EDGE + rows].astype(BF16)
            filt[:, at] = 0.5 * y.astype(F32)
            for m in range(4):
                sums[m, :, at] = product(y, diag[m, at, :])

        for lane in range(0, width, lanes):
            at = pl.ds(lane, lanes)
            rates = -0.5 * FADING_FACTOR * small_softplus(odds_ref[:, at]) * speed_ref[:, 0:1]

            def step(i, carry):
                result = []
                for d in range(2):
                    group = i if d == 0 else groups - 1 - i
                    here = pl.ds(pl.multiple_of(group * 8, 8), 8)
                    there = pl.ds(pl.multiple_of(base + group * 8, 8), 8)
                    rate = rates[d : d + 1]
                    log_keep = jnp.tanh(sums[2 * d, here, at]) * rate + rate
                    log_keep = log_keep + cols[there, d : d + 1]
                    a = jnp.exp(log_keep)
                    square = minus_tanh(log_keep) * (1.0 + a * a)
                    root = square * lax.rsqrt(square + 1e-37)
                    f = filt[here, at]
                    b = root * (f + f * jnp.tanh(sums[2 * d + 1, here, at]))
                    for k in (1, 2, 4):
                        if d == 0:
                            inside, shift = place >= k, k
                        else:
                            inside, shift = place < 8 - k, 8 - k
                        b = jnp.where(inside, b + a * pltpu.roll(b, shift, 0), b)
                        a = jnp.where(inside, a * pltpu.roll(a, shift, 0), a)
                    kept, state = carry[2 * d], carry[2 * d + 1]
                    b = b + a * state
                    a = a * kept
                    keep[d, there, at] = a
                    loc[d, there, at] = b
                    last = 7 if d == 0 else 0
                    result += [a[last : last + 1], b[last : last + 1]]
                return tuple(result)

            one, zero = jnp.ones((1, lanes), F32), jnp.zeros((1, lanes), F32)
            ends = lax.fori_loop(0, groups, step, (one, zero, one, zero), unroll=4)
            for m in range(4):
                ends_buf[owner, m : m + 1, at] = ends[m]

    far = rows * (n_tp - 1)
    total_rows = length + 2 * EDGE
    edge_at = rows + far
    loads[0].wait()
    normalise(x_own, rows, 0)
    for copy in nears:
        copy.wait_recv()
    for side in range(2):
        normalise(near.at[side], EDGE, rows + side * EDGE)

    @pl.when(jnp.logical_and(sp == 0, tp == 0))
    def _():
        normed[pl.ds(rows, EDGE), :] = jnp.zeros((EDGE, depth), BF16)

    @pl.when(jnp.logical_and(sp == n_sp - 1, tp == n_tp - 1))
    def _():
        normed[pl.ds(rows + EDGE, EDGE), :] = jnp.zeros((EDGE, depth), BF16)

    own = ((0, rows, owner_row(0)),)
    own_edges = (
        (rows, EDGE, pl.multiple_of(tp * rows, 16)),
        (rows + EDGE, EDGE, pl.multiple_of(EDGE + tp * rows + rows, 16)),
    )
    loads[1].wait()
    project(ws, s_buf, tile, 0, rows + 2 * EDGE, own + own_edges, same)
    chunk(tp)
    loads[2].wait()
    project(wg, g_buf, tile, 0, rows, own, gelu)
    loads[3].wait()
    project(wp, p_buf, ptile, 0, rows, own, same)

    for side in range(2):
        halo_copy(side, 0, 0).wait_recv()
        normalise(halo.at[side], EDGE, edge_at + side * EDGE)

    @pl.when(sp == 0)
    def _():
        normed[pl.ds(edge_at, EDGE), :] = jnp.zeros((EDGE, depth), BF16)

    @pl.when(sp == n_sp - 1)
    def _():
        normed[pl.ds(edge_at + EDGE, EDGE), :] = jnp.zeros((EDGE, depth), BF16)

    for n, copy in enumerate(gathers):
        copy.wait_recv()
        normalise(x_far, piece, rows + n * piece, n * piece)
    pieces = [((k - 1) * rows, rows, owner_row(k)) for k in range(1, n_tp)]
    edges = [(far, EDGE, 0), (far + EDGE, EDGE, EDGE + length)]
    project(ws, s_buf, tile, rows, far + 2 * EDGE, pieces + edges, same)
    for k in range(1, n_tp):
        chunk(lax.rem(tp + n_tp - k, n_tp))

    for d in range(2):
        kept, state = jnp.ones((1, width), F32), jnp.zeros((1, width), F32)
        for j in range(n_tp) if d == 0 else range(n_tp - 1, -1, -1):
            step_keep = ends_buf[j, 2 * d : 2 * d + 1, :]
            state = step_keep * state + ends_buf[j, 2 * d + 1 : 2 * d + 2, :]
            kept = step_keep * kept
        summary[d, 0:1, :] = kept
        summary[d, 1:2, :] = state

    carries = []
    for k in range(1, n_sp):
        to = lax.rem(sp + k, n_sp)
        way = jnp.where(to > sp, 0, 1)
        copy = pltpu.make_async_remote_copy(
            src_ref=summary.at[way],
            dst_ref=totals.at[k],
            send_sem=c_send.at[k],
            recv_sem=c_recv.at[k],
            device_id=(to, tp),
            device_id_type=MESH,
        )
        copy.start()
        carries.append(copy)

    project(wg, g_buf, tile, rows, far, pieces, gelu)
    project(wp, p_buf, ptile, rows, far + 2 * EDGE, pieces + edges, same)
    gw = cluster_ref.shape[1]
    local_groups = pool_width // gw
    factors = factor_ref[...].astype(F32).reshape(1, pool_width)
    position = sp * length + lax.broadcasted_iota(jnp.int32, (length, gw), 0)
    total_length = length * n_sp
    for j in range(local_groups):
        x = p_buf[:, j * gw : (j + 1) * gw]
        level = x
        code_here = lax.rem(tp * local_groups + j, 4)
        codes = (j % 4,) if local_groups % 4 == 0 else range(4)
        pooled = None
        for code in range(codes[-1] + 1):
            h = 1 << code
            level = level + pltpu.roll(level, total_rows - h, 0)
            if code not in codes:
                continue
            spanned = pltpu.roll(level, h, 0)[EDGE : EDGE + length]
            counted = jnp.minimum(position + h, total_length) - jnp.maximum(position - h, 0)
            value = spanned / counted.astype(F32)
            pooled = value if pooled is None else jnp.where(code_here == code, value, pooled)
        pooled = (pooled - x[EDGE : EDGE + length]).astype(BF16)
        mapped = product(pooled, cluster_ref[j]) * factors[:, j * gw : (j + 1) * gw]
        pool_mix[:, j * gw : (j + 1) * gw] = mapped.astype(BF16)

    for copy in carries:
        copy.wait_recv()
    forward = jnp.zeros((1, width), F32)
    backward = jnp.zeros((1, width), F32)
    for k in range(n_sp - 1, 0, -1):
        valid = k <= sp
        forward = jnp.where(valid, totals[k, 0:1, :] * forward + totals[k, 1:2, :], forward)
    for k in range(1, n_sp):
        valid = k > sp
        backward = jnp.where(valid, totals[k, 0:1, :] * backward + totals[k, 1:2, :], backward)

    for j in range(n_tp):
        carry_in[j, 0:1, :] = forward
        forward = ends_buf[j, 0:1, :] * forward + ends_buf[j, 1:2, :]
    for j in range(n_tp - 1, -1, -1):
        carry_in[j, 1:2, :] = backward
        backward = ends_buf[j, 2:3, :] * backward + ends_buf[j, 3:4, :]

    loads[4].wait()
    loads[5].wait()
    columns = wso.shape[1]
    parts = part.shape[1]
    ctile = columns // parts

    def mix_rows(owner):
        first = owner * rows
        forward = carry_in[owner, 0:1, :]
        backward = carry_in[owner, 1:2, :]

        @pl.loop(0, rows // 16)
        def _(i):
            here = pl.ds(pl.multiple_of(first + i * 16, 16), 16)
            state = loc[0, here, :] + keep[0, here, :] * forward
            state = state + loc[1, here, :] + keep[1, here, :] * backward
            gate = g_buf[pl.ds(pl.multiple_of(EDGE + first + i * 16, 16), 16), :]
            mix[here, :] = (gate * state).astype(BF16)

    def share(first, c):
        here = pl.ds(first, rows)
        at = pl.ds(c * ctile, ctile)
        return product(mix[here, :], wso[:, at]) + product(pool_mix[here, :], wpo[:, at])

    scatters = []
    for k in range(1, n_tp):
        to = lax.rem(tp + k, n_tp)
        first = pl.multiple_of(to * rows, 16)
        mix_rows(to)
        for c in range(parts):
            part[k - 1, c] = share(first, c).astype(BF16)
            scatters.append(
                pltpu.make_async_remote_copy(
                    src_ref=part.at[k - 1, c],
                    dst_ref=landed.at[k - 1, c],
                    send_sem=rs_send.at[k - 1, c],
                    recv_sem=rs_recv.at[k - 1, c],
                    device_id=(sp, to),
                    device_id_type=MESH,
                )
            )
            if len(scatters) > 1:
                scatters[-2].start()
    first = pl.multiple_of(tp * rows, 16)
    mix_rows(tp)
    if scatters:
        scatters[-1].start()
    for c in range(parts):
        x_total = share(first, c)
        for k in range(1, n_tp):
            scatters[(k - 1) * parts + c].wait_recv()
            x_total = x_total + landed[k - 1, c].astype(F32)
        out_ref[:, c * ctile : (c + 1) * ctile] = x_total.astype(BF16)

    for copy in gathers + nears + carries + scatters:
        copy.wait_send()
    for side, sender in ((0, n_tp - 1), (1, 0)):

        @pl.when(tp == sender)
        def _():
            for j in range(n_tp):
                halo_copy(side, j, j).wait_send()


def local(
    n_sp,
    n_tp,
    incoming_activity,
    entry_standardize_factor,
    recursive_entry_matrix,
    final_switch_matrix,
    averaging_entry_matrix,
    percolumn_filter_coefficients,
    switch_tiled_matrices,
    prior_fading_odds,
    speed_factors,
    extra_fading_amounts,
    averaging_cluster_matrices,
    averaging_feature_factor,
    recursive_final_matrix,
    averaging_final_matrix,
):
    rows, depth = incoming_activity.shape
    length = rows * n_tp
    width = recursive_entry_matrix.shape[1]
    pool_width = averaging_entry_matrix.shape[1]
    columns = recursive_final_matrix.shape[1]
    half = switch_tiled_matrices.shape[-1]
    parts = 4
    tile = min(256, width)
    hbm = pl.BlockSpec(memory_space=pl.ANY)
    vmem = pl.BlockSpec(memory_space=pltpu.VMEM)
    dma = pltpu.SemaphoreType.DMA
    peers = max(n_tp - 1, 1)
    padded = length + 2 * EDGE
    return pl.pallas_call(
        functools.partial(kernel, n_sp, n_tp),
        out_shape=jax.ShapeDtypeStruct((rows, columns), BF16),
        in_specs=[hbm, vmem, hbm, hbm, hbm, vmem, vmem, vmem, vmem, vmem, vmem, vmem, hbm, hbm],
        out_specs=vmem,
        scratch_shapes=[
            pltpu.VMEM((rows, depth), BF16),
            pltpu.VMEM((rows * peers, depth), BF16),
            pltpu.VMEM((2, EDGE, depth), BF16),
            pltpu.VMEM((2, EDGE, depth), BF16),
            pltpu.VMEM((length, 8), F32),
            pltpu.VMEM((padded, depth), BF16),
            pltpu.VMEM((depth, width), BF16),
            pltpu.VMEM((depth, width), BF16),
            pltpu.VMEM((depth, pool_width), BF16),
            pltpu.VMEM((width, columns), BF16),
            pltpu.VMEM((pool_width, columns), BF16),
            pltpu.VMEM((padded, width), F32),
            pltpu.VMEM((padded, width), F32),
            pltpu.VMEM((padded, pool_width), F32),
            pltpu.VMEM((rows, width), F32),
            pltpu.VMEM((4, width, tile), BF16),
            pltpu.VMEM((4, rows, width), F32),
            pltpu.VMEM((2, length, width), F32),
            pltpu.VMEM((2, length, width), F32),
            pltpu.VMEM((n_tp, 4, width), F32),
            pltpu.VMEM((n_tp, 2, width), F32),
            pltpu.VMEM((2, 2, width), F32),
            pltpu.VMEM((n_sp, 2, width), F32),
            pltpu.VMEM((length, width), BF16),
            pltpu.VMEM((length, pool_width), BF16),
            pltpu.VMEM((peers, parts, rows, columns // parts), BF16),
            pltpu.VMEM((peers, parts, rows, columns // parts), BF16),
            dma((6,)),
            dma((n_tp, 4)),
            dma((n_tp, 4)),
            dma((2, n_tp)),
            dma((2,)),
            dma((2,)),
            dma((2,)),
            dma((n_sp,)),
            dma((n_sp,)),
            dma((peers, parts)),
            dma((peers, parts)),
        ],
        compiler_params=pltpu.CompilerParams(
            has_side_effects=True, vmem_limit_bytes=63 * 1024 * 1024
        ),
    )(
        incoming_activity,
        entry_standardize_factor,
        recursive_entry_matrix,
        final_switch_matrix,
        averaging_entry_matrix,
        percolumn_filter_coefficients,
        switch_tiled_matrices.reshape(4, width, half),
        prior_fading_odds,
        speed_factors,
        extra_fading_amounts,
        averaging_cluster_matrices,
        averaging_feature_factor,
        recursive_final_matrix,
        averaging_final_matrix,
    )


def solution(mesh):
    in_specs = (
        P(("sp", "tp"), None),
        P(),
        P(None, "tp"),
        P(None, "tp"),
        P(None, "tp"),
        P(None, "tp"),
        P(None, None, "tp", None, None),
        P(None, "tp"),
        P(None, "sp"),
        P(None, "sp"),
        P("tp", None, None),
        P("tp"),
        P("tp", None),
        P("tp", None),
    )
    out_specs = P(("sp", "tp"), None)
    body = functools.partial(local, mesh.shape["sp"], mesh.shape["tp"])
    return jax.shard_map(body, mesh=mesh, in_specs=in_specs, out_specs=out_specs, check_vma=False)
```
